32 devices in a mesh: sp: 8 (over z, y), tp: 4 (over x, core).
Axes of the slice: x: 2, y: 2, z: 4, core: 2. Of those that a mesh axis runs over, the one named last changes fastest.
Arguments:
- tokens: bfloat16 [2048, 2048], P('sp', 'tp'), may hold values from -19 to 250
- in_gain: bfloat16 [2048], replicated, may hold values from 0.099609375 to 1.8984375
- w_glu_value: bfloat16 [2048, 512], P(None, 'tp'), may hold values from -0.125 to 0.125
- w_glu_gate: bfloat16 [2048, 512], P(None, 'tp'), may hold values from -0.125 to 0.125
- w_query: bfloat16 [2048, 1024], P(None, 'tp'), may hold values from -1 to 1
- w_key: bfloat16 [2048, 512], P(None, 'tp'), may hold values from -1 to 1
- w_value: bfloat16 [2048, 512], P(None, 'tp'), may hold values from -0.125 to 0.125
- w_gate_conv: bfloat16 [2048, 512], P(None, 'tp'), may hold values from -0.125 to 0.125
- w_gate_attn: bfloat16 [2048, 1024], P(None, 'tp'), may hold values from -0.125 to 0.125
- conv_weight: bfloat16 [31, 512], P(None, 'tp'), may hold values from -4.6 to 4.6
- conv_gain: float32 [512], P('tp'), may hold values from 0.1 to 1.9
- lam: float32 [8], P('tp'), may hold values from 0.3 to 0.8
- head_gain: float32 [128], replicated, may hold values from 0.1 to 1.9
- out_conv: bfloat16 [512, 2048], P('tp'), may hold values from -0.15625 to 0.15625
- out_attn: bfloat16 [1024, 2048], P('tp'), may hold values from -0.15625 to 0.15625
Outputs:
- mixed: bfloat16 [2048, 2048], P(('sp', 'tp'))
The draws below stay inside these ranges and needn't reach their ends.
All inputs are finite; a program needn't handle non-finite values.
Results may differ from the reference program's by a relative error of at most 0.017.
The reference program's roundings to bfloat16 on the way count: a program that leaves them out, or rounds other values in their place, can miss the bound.
Values may be sent and summed in bfloat16 or wider, within the bound.
A program may use at most 128 MiB of HBM per device.

```python
import math
import jax
import jax.numpy as jnp
from jax import lax

D = 2048
CONV = 512
HEADS = 8
KV_HEADS = 4
QK = 64
VDIM = 128
WIDTH = 31
TOKENS = 2048
N_TP = 4


def draw_tokens(key, part):
    k_base = jax.random.fold_in(jax.random.fold_in(key, 11), 0)
    values = jnp.clip(jax.random.normal(k_base, (TOKENS, D), jnp.float32), -6.0, 6.0)
    return values.astype(jnp.bfloat16)


def draw_w_query(key, part):
    values = jnp.clip(jax.random.normal(jax.random.fold_in(key, 21), (D, HEADS * 2 * QK), jnp.float32), -6.0, 6.0)
    values = values * (1.3 / jnp.sqrt(jnp.float32(D)))
    return values.astype(jnp.bfloat16)


def draw_w_key(key, part):
    values = jnp.clip(jax.random.normal(jax.random.fold_in(key, 22), (D, KV_HEADS * 2 * QK), jnp.float32), -6.0, 6.0)
    values = values * (1.3 / jnp.sqrt(jnp.float32(D)))
    return values.astype(jnp.bfloat16)


def draw_conv_weight(key, part):
    k_base, k_rough = jax.random.split(jax.random.fold_in(key, 31), 2)
    position = jnp.arange(CONV, dtype=jnp.float32) / CONV
    trend = 3.0 ** (position - 0.5)
    rough = jnp.exp(jax.random.uniform(k_rough, (CONV,), jnp.float32, -0.7, 0.7))
    values = jnp.clip(jax.random.normal(k_base, (WIDTH, CONV), jnp.float32), -4.0, 4.0)
    values = values / jnp.sqrt(jnp.float32(WIDTH)) * (trend * rough)[None, :]
    return values.astype(jnp.bfloat16)


def shard_levels(stream_key, shape, cuts, smallest, largest):
    gain, own = 1.0, jax.random.fold_in(stream_key, 6)
    for dim, parts in cuts:
        heights = jnp.exp(jax.random.uniform(jax.random.fold_in(own, dim), (parts,), jnp.float32, smallest / len(cuts), largest / len(cuts)))
        gain = gain * jnp.repeat(heights, shape[dim] // parts).reshape([-1 if axis == dim else 1 for axis in range(len(shape))])
    return gain


def gaussian(rng, shape, deviation, reach, cuts=(), kind=jnp.bfloat16):
    level = shard_levels(rng, shape, cuts, -0.22, 0.18) if cuts else 1.0
    entries = jax.random.normal(rng, shape, jnp.float32) * deviation * level
    return jnp.minimum(jnp.maximum(entries, -reach), reach).astype(kind)


def setup_inputs(seed: int = 0) -> dict:
    streams_of = jax.random.split(jax.random.key(seed), 16)
    return {
        "tokens": draw_tokens(jax.random.fold_in(streams_of[15], 71), 0),
        "in_gain": jnp.clip(1.0 + 0.18 * jax.random.normal(streams_of[1], (D,), jnp.float32), 0.099609375, 1.8984375).astype(jnp.bfloat16),
        "w_glu_value": gaussian(streams_of[2], (D, CONV), D ** -0.5, 0.125, ((1, 4),)),
        "w_glu_gate": gaussian(streams_of[3], (D, CONV), D ** -0.5, 0.125, ((1, 4),)),
        "w_query": draw_w_query(jax.random.fold_in(streams_of[15], 71), 0),
        "w_key": draw_w_key(jax.random.fold_in(streams_of[15], 71), 0),
        "w_value": gaussian(streams_of[6], (D, KV_HEADS * VDIM), D ** -0.5, 0.125, ((1, 4),)),
        "w_gate_conv": gaussian(streams_of[7], (D, CONV), D ** -0.5, 0.125, ((1, 4),)),
        "w_gate_attn": gaussian(streams_of[8], (D, HEADS * VDIM), D ** -0.5, 0.125, ((1, 4),)),
        "conv_weight": draw_conv_weight(jax.random.fold_in(streams_of[15], 71), 0),
        "conv_gain": jnp.clip(1.0 + 0.18 * jax.random.normal(streams_of[10], (CONV,), jnp.float32), 0.1, 1.9),
        "lam": jnp.clip(0.3 + 0.5 * jax.random.uniform(streams_of[11], (HEADS,), jnp.float32) ** shard_levels(streams_of[11], (HEADS,), ((0, 4),), -0.2, 0.2), 0.3, 0.8),
        "head_gain": jnp.clip(1.0 + 0.18 * jax.random.normal(streams_of[12], (VDIM,), jnp.float32), 0.1, 1.9),
        "out_conv": gaussian(streams_of[13], (CONV, D), (CONV + HEADS * VDIM) ** -0.5, 0.15625, ((0, 4),)),
        "out_attn": gaussian(streams_of[14], (HEADS * VDIM, D), (CONV + HEADS * VDIM) ** -0.5, 0.15625, ((0, 4),)),
    }


EPSILON = 1e-06
NEG_BIG = -1e+30
HEAD_SCALE = 0.8

def attend_head(query_head, key_head, value_head, lam_head, head_gain):
    block_rows = math.gcd(TOKENS, 512)
    blocks = TOKENS // block_rows
    scale_factor = 1.0 / math.sqrt(QK)

    def one_block(index):
        query_block = lax.dynamic_slice_in_dim(query_head, index * block_rows, block_rows, 0).astype(jnp.float32)
        query_pos = index * block_rows + jnp.arange(block_rows, dtype=jnp.int32)

        def visit(other, running):
            maxima, totals, summed = running
            key_block = lax.dynamic_slice_in_dim(key_head, other * block_rows, block_rows, 0).astype(jnp.float32)
            value_block = lax.dynamic_slice_in_dim(value_head, other * block_rows, block_rows, 0).astype(jnp.float32)
            scores = jnp.einsum('qcd,kcd->cqk', query_block, key_block) * scale_factor
            key_pos = other * block_rows + jnp.arange(block_rows, dtype=jnp.int32)
            scores = jnp.where(key_pos[None, None, :] <= query_pos[None, :, None], scores, NEG_BIG)
            new_max = jnp.maximum(maxima, lax.optimization_barrier(jnp.max(scores, axis=2)))
            factor = jnp.exp(maxima - new_max)
            expd = jnp.exp(scores - new_max[:, :, None])
            totals = totals * factor + lax.optimization_barrier(jnp.sum(expd, axis=2))
            rounded = lax.optimization_barrier(expd.astype(jnp.bfloat16)).astype(jnp.float32)
            summed = summed * factor[:, :, None] + jnp.einsum('cqk,kv->cqv', rounded, value_block)
            return (new_max, totals, summed)
        start_state = (jnp.full((2, block_rows), NEG_BIG, jnp.float32), jnp.zeros((2, block_rows), jnp.float32), jnp.zeros((2, block_rows, VDIM), jnp.float32))
        maxima, totals, summed = lax.fori_loop(0, index + 1, visit, start_state)
        output = summed[0] / totals[0][:, None] - lam_head * summed[1] / totals[1][:, None]
        normed = output * lax.rsqrt(lax.optimization_barrier(jnp.mean(output * output, axis=1, keepdims=True)) + EPSILON)
        return normed * head_gain[None, :] * HEAD_SCALE
    result = lax.map(one_block, jnp.arange(blocks, dtype=jnp.int32))
    return result.reshape(TOKENS, VDIM)

def reference(tokens, in_gain, w_glu_value, w_glu_gate, w_query, w_key, w_value, w_gate_conv, w_gate_attn, conv_weight, conv_gain, lam, head_gain, out_conv, out_attn):
    widened = tokens.astype(jnp.float32)
    inv_rms = lax.rsqrt(lax.optimization_barrier(jnp.mean(widened * widened, axis=1, keepdims=True)) + EPSILON)
    scaled = (widened * in_gain.astype(jnp.float32)[None, :]).astype(jnp.bfloat16)

    def project(weight):
        return (jnp.dot(scaled, weight, preferred_element_type=jnp.float32) * inv_rms).astype(jnp.bfloat16)
    glu_value = project(w_glu_value)
    glu_gate = project(w_glu_gate)
    query = project(w_query)
    key = project(w_key)
    value = project(w_value)
    gate_conv = project(w_gate_conv)
    gate_attn = project(w_gate_attn)
    glued = (glu_value.astype(jnp.float32) * jax.nn.sigmoid(glu_gate.astype(jnp.float32))).astype(jnp.bfloat16)
    padded = jnp.pad(glued.astype(jnp.float32), ((WIDTH - 1, 0), (0, 0)))
    taps = conv_weight.astype(jnp.float32)
    conv = jnp.zeros((TOKENS, CONV), jnp.float32)
    for offset in range(WIDTH):
        conv = conv + padded[offset:offset + TOKENS] * taps[offset][None, :]
    channel_ms = lax.optimization_barrier(jnp.mean(conv * conv, axis=1, keepdims=True))
    conv_normed = conv * lax.rsqrt(channel_ms + EPSILON) * conv_gain[None, :]
    y_conv = (jax.nn.silu(conv_normed) * jax.nn.silu(gate_conv.astype(jnp.float32))).astype(jnp.bfloat16)
    group = HEADS // KV_HEADS
    query_heads = jnp.transpose(query.reshape(TOKENS, HEADS, 2, QK), (1, 0, 2, 3))
    key_heads = jnp.transpose(key.reshape(TOKENS, KV_HEADS, 2, QK), (1, 0, 2, 3))
    value_heads = jnp.transpose(value.reshape(TOKENS, KV_HEADS, VDIM), (1, 0, 2))

    def per_head(head):
        shared = head // group
        return attend_head(query_heads[head], key_heads[shared], value_heads[shared], lam[head], head_gain)
    heads_out = lax.map(per_head, jnp.arange(HEADS, dtype=jnp.int32))
    attn_normed = jnp.transpose(heads_out, (1, 0, 2)).reshape(TOKENS, HEADS * VDIM)
    y_attn = (attn_normed * jax.nn.silu(gate_attn.astype(jnp.float32))).astype(jnp.bfloat16)
    conv_block = CONV // N_TP
    attn_block = HEADS * VDIM // N_TP
    mixed = jnp.zeros((TOKENS, D), jnp.float32)
    for member in range(N_TP):
        partial_value = jnp.dot(y_conv[:, member * conv_block:(member + 1) * conv_block], out_conv[member * conv_block:(member + 1) * conv_block], preferred_element_type=jnp.float32)
        partial_value = partial_value + jnp.dot(y_attn[:, member * attn_block:(member + 1) * attn_block], out_attn[member * attn_block:(member + 1) * attn_block], preferred_element_type=jnp.float32)
        mixed = mixed + lax.optimization_barrier(partial_value.astype(jnp.bfloat16)).astype(jnp.float32)
    return mixed.astype(jnp.bfloat16)
```

```python
import functools
import math

import jax
import jax.numpy as jnp
from jax import lax
from jax.experimental import pallas as pl
from jax.experimental.pallas import tpu as pltpu
from jax.sharding import PartitionSpec as P

EPSILON = 1e-06
NEG_BIG = -1e30
HEAD_SCALE = 0.8
QK = 64
VDIM = 128
MESH = pl.DeviceIdType.MESH
F32 = jnp.float32
BF16 = jnp.bfloat16
PIECES = 4
PAD = 32


def dot(a, b, ca=1, cb=0, precision=None):
    return lax.dot_general(
        a, b, (((ca,), (cb,)), ((), ())), preferred_element_type=F32, precision=precision
    )


def kernel(
    n_sp,
    n_tp,
    tok,
    gain,
    w_glu_value,
    w_glu_gate,
    w_query,
    w_key,
    w_value,
    w_gate_conv,
    w_gate_attn,
    taps_ref,
    conv_gain,
    lam,
    head_gain,
    out_conv,
    out_attn,
    out,
    w_all,
    w_out,
    tokbuf,
    acc,
    kbuf,
    vbuf,
    q4,
    m_ref,
    l_ref,
    o_ref,
    gl,
    tail_out,
    tail_in,
    sq_out,
    sq_in,
    ybuf,
    a_out,
    a_own,
    a_in,
    x_out,
    x_in,
    b_out,
    b_own,
    b_in,
    w_sem,
    tok_send,
    tok_recv,
    kv_recv,
    up_send,
    side_send,
    tail_sem,
    sq_send,
    sq_recv,
    a_sem,
    x_sem,
    b_sem,
):
    rows, depth = tok.shape
    width = depth * n_tp
    s = lax.axis_index("sp")
    t = lax.axis_index("tp")
    core = t % 2
    p1 = t + 1 - 2 * core
    p2 = (t + 2) % n_tp
    p3 = (p1 + 2) % n_tp
    y = s % 2
    z = s // 2
    mate = s + 1 - 2 * y
    has_up = s + 2 < n_sp

    weights = (w_key, w_value, w_glu_value, w_glu_gate, w_query, w_gate_conv, w_gate_attn)
    spans = []
    at = 0
    loads = []
    for i, w in enumerate(weights):
        cols = w.shape[1]
        spans.append((at, at + cols))
        loads.append(pltpu.make_async_copy(w, w_all.at[:, at : at + cols], w_sem.at[i]))
        at += cols
    total_cols = at
    at = 0
    out_loads = []
    for i, w in enumerate((out_conv, out_attn)):
        r = w.shape[0]
        out_loads.append(
            pltpu.make_async_copy(w, w_out.at[at : at + r, :], w_sem.at[len(weights) + i])
        )
        at += r
    for copy in loads + out_loads:
        copy.start()

    def tp_copy(src, dst, send, recv, to):
        return pltpu.make_async_remote_copy(
            src_ref=src, dst_ref=dst, send_sem=send, recv_sem=recv,
            device_id={"tp": to}, device_id_type=MESH,
        )

    def sp_copy(src, dst, send, recv, to):
        return pltpu.make_async_remote_copy(
            src_ref=src, dst_ref=dst, send_sem=send, recv_sem=recv,
            device_id={"sp": to}, device_id_type=MESH,
        )

    barrier = pltpu.get_barrier_semaphore()
    for peer in (p1, p2, p3):
        pl.semaphore_signal(barrier, inc=1, device_id={"tp": peer}, device_id_type=MESH)
    for by in (-2, -1, 1, 2):
        other = s + by

        @pl.when((other >= 0) & (other < n_sp))
        def _():
            pl.semaphore_signal(barrier, inc=1, device_id={"sp": other}, device_id_type=MESH)

    pl.semaphore_wait(barrier, 3 + jnp.minimum(s, 2) + jnp.minimum(n_sp - 1 - s, 2))

    half = rows // 2
    across = [
        tp_copy(
            tok.at[c * half : (c + 1) * half], tokbuf.at[1, c * half : (c + 1) * half],
            tok_send.at[c], tok_recv.at[c], p2,
        )
        for c in range(2)
    ]
    beside = tp_copy(tok, tokbuf.at[0], tok_send.at[2], tok_recv.at[2], p1)
    passed = [
        tp_copy(
            tokbuf.at[1, c * half : (c + 1) * half], tokbuf.at[2, c * half : (c + 1) * half],
            tok_send.at[3 + c], tok_recv.at[3 + c], p1,
        )
        for c in range(2)
    ]
    for copy in across:
        copy.start()
    beside.start()

    def prepare(x, owner):
        wide = x.astype(F32)
        first = pl.multiple_of(owner * depth, depth)
        g = gain[:, pl.ds(first, depth)].astype(F32)
        return (wide * g).astype(BF16), jnp.sum(wide * wide, axis=1, keepdims=True), first

    scaled, squares, first = prepare(tok[...], t)
    for copy in loads:
        copy.wait()
    acc[...] = dot(scaled, w_all[pl.ds(first, depth), :])
    beside.wait_recv()
    scaled, more, first = prepare(tokbuf[0], p1)
    squares = squares + more
    acc[...] += dot(scaled, w_all[pl.ds(first, depth), :])
    for c in range(2):
        across[c].wait_recv()
        passed[c].start()
    scaled, more, first = prepare(tokbuf[1], p2)
    squares = squares + more
    acc[...] += dot(scaled, w_all[pl.ds(first, depth), :])
    for c in range(2):
        passed[c].wait_recv()
    scaled, more, first = prepare(tokbuf[2], p3)
    squares = squares + more
    inv_rms = lax.rsqrt(squares / width + EPSILON)
    early = spans[3][1]
    acc[:, :early] += dot(scaled, w_all[pl.ds(first, depth), :early])

    def projected(i, lo=0, hi=None):
        hi = rows if hi is None else hi
        a, b = spans[i]
        return (acc[lo:hi, a:b] * inv_rms[lo:hi]).astype(BF16)

    def glue(lo, hi):
        value = projected(2, lo, hi).astype(F32)
        gate = projected(3, lo, hi).astype(F32)
        return (value * jax.nn.sigmoid(gate)).astype(BF16)

    tail_out[...] = glue(rows - PAD, rows)
    tail = sp_copy(tail_out, tail_in, tail_sem.at[0], tail_sem.at[1], s + 1)

    @pl.when(s + 1 < n_sp)
    def _():
        tail.start()

    def up(j, c):
        buf = (kbuf, vbuf)[c]
        return sp_copy(buf.at[j], buf.at[j], up_send.at[j, c], kv_recv.at[j, c], s + 2)

    def side(j, c):
        buf = (kbuf, vbuf)[c]
        return sp_copy(buf.at[j], buf.at[j], side_send.at[j, c], kv_recv.at[j, c], mate)

    kbuf[s] = projected(0)
    vbuf[s] = jnp.transpose(projected(1).astype(F32)).astype(BF16)
    for c in range(2):

        @pl.when(has_up)
        def _():
            up(s, c).start()

        @pl.when(y == 0)
        def _():
            side(s, c).start()

    acc[:, early:] += dot(scaled, w_all[pl.ds(first, depth), early:])
    query = projected(4).astype(F32) * (1.0 / math.sqrt(QK))
    heads = w_query.shape[1] // (2 * QK)
    lane = lax.broadcasted_iota(jnp.int32, (rows, 2 * QK), 1)
    for h in range(heads):
        qh = query[:, h * 2 * QK : (h + 1) * 2 * QK]
        for m in range(2):
            keep = (lane >= m * QK) & (lane < (m + 1) * QK)
            q4[2 * h + m] = jnp.where(keep, qh, 0.0).astype(BF16)
    gl[PAD:, :] = glue(0, rows).astype(F32)

    key_pos = lax.broadcasted_iota(jnp.int32, (rows, rows), 0)
    query_pos = lax.broadcasted_iota(jnp.int32, (rows, rows), 1)
    allowed = key_pos <= query_pos
    k = kbuf[s]
    v = vbuf[s]
    for i in range(2 * heads):
        scores = jnp.where(allowed, dot(k, q4[i], 1, 1), NEG_BIG)
        top = jnp.max(scores, axis=0, keepdims=True)
        e = jnp.exp(scores - top)
        m_ref[i] = top
        l_ref[i] = jnp.sum(e, axis=0, keepdims=True)
        o_ref[i] = dot(v, e.astype(BF16))

    @pl.when(s == 0)
    def _():
        gl[:PAD, :] = jnp.zeros((PAD, gl.shape[1]), F32)

    @pl.when(s > 0)
    def _():
        tail.wait_recv()
        gl[:PAD, :] = tail_in[...].astype(F32)

    n_taps = taps_ref.shape[0]
    taps = taps_ref[...].astype(F32)
    conv = jnp.zeros((rows, gl.shape[1]), F32)
    for j in range(n_taps):
        lo = PAD - (n_taps - 1) + j
        conv = conv + gl[lo : lo + rows, :] * taps[j : j + 1, :]
    ones = jnp.ones((8, conv.shape[1]), F32)
    high = lax.Precision.HIGHEST
    sq_out[...] = dot(ones, conv * conv, 1, 1, high)
    sq_copies = [
        tp_copy(sq_out, sq_in.at[i], sq_send.at[i], sq_recv.at[i], p)
        for i, p in enumerate((p1, p2, p3))
    ]
    for copy in sq_copies:
        copy.start()

    def visit(j):
        k = kbuf[j]
        v = vbuf[j]
        for i in range(2 * heads):
            scores = dot(k, q4[i], 1, 1)
            old = m_ref[i]
            top = jnp.maximum(old, jnp.max(scores, axis=0, keepdims=True))
            factor = jnp.exp(old - top)
            e = jnp.exp(scores - top)
            m_ref[i] = top
            l_ref[i] = l_ref[i] * factor + jnp.sum(e, axis=0, keepdims=True)
            o_ref[i] = o_ref[i] * factor + dot(v, e.astype(BF16))

    gate_conv = projected(5).astype(F32)
    for copy in sq_copies:
        copy.wait_recv()
    total_sq = sq_out[...] + sq_in[0] + sq_in[1] + sq_in[2]
    spread = jnp.full((8, conv.shape[1]), 0.125, F32)
    conv_all = conv.shape[1] * n_tp
    mean_sq = dot(total_sq, spread, 0, 0, high) / conv_all
    normed = conv * lax.rsqrt(mean_sq + EPSILON) * conv_gain[...]
    conv_local = conv.shape[1]
    ybuf[:, :conv_local] = (
        normed * jax.nn.sigmoid(normed) * (gate_conv * jax.nn.sigmoid(gate_conv))
    ).astype(BF16)

    @pl.when(y == 1)
    def _():
        for c in range(2):
            side(mate, c).wait_recv()
        visit(mate)

    def step(i, carry):
        k = i + 1
        j = s - 2 * k
        for c in range(2):
            up(j, c).wait_recv()

            @pl.when(has_up)
            def _():
                up(j, c).start()

            side(j, c).start()
        visit(j)
        other = mate - 2 * k
        for c in range(2):
            side(other, c).wait_recv()
        visit(other)
        return carry

    lax.fori_loop(0, z, step, 0)

    for h in range(heads):
        first_map = o_ref[2 * h] / l_ref[2 * h]
        second_map = o_ref[2 * h + 1] / l_ref[2 * h + 1]
        o = first_map - lam[h] * second_map
        n = o * lax.rsqrt(jnp.mean(o * o, axis=0, keepdims=True) + EPSILON)
        a, b = spans[6]
        lo = a + h * VDIM
        gate = (acc[:, lo : lo + VDIM] * inv_rms).astype(BF16).astype(F32)
        n = jnp.transpose(n) * head_gain[...] * HEAD_SCALE
        at = conv_local + h * VDIM
        ybuf[:, at : at + VDIM] = (n * (gate * jax.nn.sigmoid(gate))).astype(BF16)

    for copy in out_loads:
        copy.wait()
    part = rows // n_tp

    def block(p):
        return ybuf[pl.ds(pl.multiple_of(p * part, part), part), :]

    cols = w_out.shape[1] // PIECES
    far = jnp.concatenate([block(p3), block(p2)], axis=0)
    a_copies = []
    for c in range(PIECES):
        r = dot(far, w_out[:, c * cols : (c + 1) * cols]).astype(BF16)
        a_out[c] = r[:part]
        a_own[c] = r[part:]
        copy = tp_copy(a_out.at[c], a_in.at[c], a_sem.at[0, c], a_sem.at[1, c], p1)
        copy.start()
        a_copies.append(copy)
    x_copies = []
    for c in range(PIECES):
        a_copies[c].wait_recv()
        x_out[c] = (a_own[c].astype(F32) + a_in[c].astype(F32)).astype(BF16)
        copy = tp_copy(x_out.at[c], x_in.at[c], x_sem.at[0, c], x_sem.at[1, c], p2)
        copy.start()
        x_copies.append(copy)
    near = jnp.concatenate([block(p1), block(t)], axis=0)
    b_copies = []
    for c in range(PIECES):
        r = dot(near, w_out[:, c * cols : (c + 1) * cols]).astype(BF16)
        b_out[c] = r[:part]
        b_own[c] = r[part:]
        copy = tp_copy(b_out.at[c], b_in.at[c], b_sem.at[0, c], b_sem.at[1, c], p1)
        copy.start()
        b_copies.append(copy)
    for c in range(PIECES):
        b_copies[c].wait_recv()
        x_copies[c].wait_recv()
        out[:, c * cols : (c + 1) * cols] = (
            b_own[c].astype(F32) + b_in[c].astype(F32) + x_in[c].astype(F32)
        ).astype(BF16)

    for copy in across + [beside] + passed + sq_copies + a_copies + x_copies + b_copies:
        copy.wait_send()

    @pl.when(s + 1 < n_sp)
    def _():
        tail.wait_send()

    for c in range(2):

        @pl.when(has_up)
        def _():
            up(s, c).wait_send()

        @pl.when(y == 0)
        def _():
            side(s, c).wait_send()

    def drain(i, carry):
        j = s - 2 * (i + 1)
        for c in range(2):

            @pl.when(has_up)
            def _():
                up(j, c).wait_send()

            side(j, c).wait_send()
        return carry

    lax.fori_loop(0, z, drain, 0)


def local(n_sp, n_tp, *args):
    (tokens, in_gain, w_glu_value, w_glu_gate, w_query, w_key, w_value, w_gate_conv,
     w_gate_attn, conv_weight, conv_gain, lam, head_gain, out_conv, out_attn) = args
    rows, depth = tokens.shape
    width = depth * n_tp
    weights = (w_glu_value, w_glu_gate, w_query, w_key, w_value, w_gate_conv, w_gate_attn)
    total_cols = sum(w.shape[1] for w in weights)
    out_rows = out_conv.shape[0] + out_attn.shape[0]
    out_cols = out_conv.shape[1]
    conv_local = conv_weight.shape[1]
    heads = lam.shape[0]
    part = rows // n_tp
    cols = out_cols // PIECES
    vmem = pl.BlockSpec(memory_space=pltpu.VMEM)
    hbm = pl.BlockSpec(memory_space=pl.ANY)
    smem = pl.BlockSpec(memory_space=pltpu.SMEM)
    dma = pltpu.SemaphoreType.DMA
    piece = pltpu.VMEM((PIECES, part, cols), BF16)
    return pl.pallas_call(
        functools.partial(kernel, n_sp, n_tp),
        out_shape=jax.ShapeDtypeStruct((part, out_cols), BF16),
        in_specs=[vmem, vmem] + [hbm] * 7 + [vmem, vmem, smem, vmem, hbm, hbm],
        out_specs=vmem,
        scratch_shapes=[
            pltpu.VMEM((width, total_cols), BF16),
            pltpu.VMEM((out_rows, out_cols), BF16),
            pltpu.VMEM((3, rows, depth), BF16),
            pltpu.VMEM((rows, total_cols), F32),
            pltpu.VMEM((n_sp, rows, 2 * QK), BF16),
            pltpu.VMEM((n_sp, VDIM, rows), BF16),
            pltpu.VMEM((2 * heads, rows, 2 * QK), BF16),
            pltpu.VMEM((2 * heads, 1, rows), F32),
            pltpu.VMEM((2 * heads, 1, rows), F32),
            pltpu.VMEM((2 * heads, VDIM, rows), F32),
            pltpu.VMEM((PAD + rows, conv_local), F32),
            pltpu.VMEM((PAD, conv_local), BF16),
            pltpu.VMEM((PAD, conv_local), BF16),
            pltpu.VMEM((8, rows), F32),
            pltpu.VMEM((3, 8, rows), F32),
            pltpu.VMEM((rows, out_rows), BF16),
            piece, piece, piece, piece, piece, piece, piece, piece,
            dma((9,)),
            dma((5,)),
            dma((5,)),
            dma((n_sp, 2)),
            dma((n_sp, 2)),
            dma((n_sp, 2)),
            dma((2,)),
            dma((3,)),
            dma((3,)),
            dma((2, PIECES)),
            dma((2, PIECES)),
            dma((2, PIECES)),
        ],
        compiler_params=pltpu.CompilerParams(
            collective_id=0, has_side_effects=True, vmem_limit_bytes=60 * 1024 * 1024
        ),
    )(
        tokens, in_gain.reshape(1, width), w_glu_value, w_glu_gate, w_query, w_key, w_value,
        w_gate_conv, w_gate_attn, conv_weight, conv_gain.reshape(1, conv_local), lam,
        head_gain.reshape(1, VDIM), out_conv, out_attn,
    )


def solution(mesh):
    n_sp, n_tp = mesh.shape["sp"], mesh.shape["tp"]
    assert n_tp == 4 and n_sp % 2 == 0
    col = P(None, "tp")
    in_specs = (
        P("sp", "tp"), P(), col, col, col, col, col, col, col, col,
        P("tp"), P("tp"), P(), P("tp", None), P("tp", None),
    )
    return jax.shard_map(
        functools.partial(local, n_sp, n_tp), mesh=mesh, in_specs=in_specs,
        out_specs=P(("sp", "tp"), None), check_vma=False,
    )
```

```python
import functools
import math

import jax
import jax.numpy as jnp
from jax import lax
from jax.experimental import pallas as pl
from jax.experimental.pallas import tpu as pltpu
from jax.sharding import PartitionSpec as P

EPSILON = 1e-06
NEG_BIG = -1e30
HEAD_SCALE = 0.8
QK = 64
VDIM = 128
MESH = pl.DeviceIdType.MESH
F32 = jnp.float32
BF16 = jnp.bfloat16
PIECES = 4
PAD = 32
LANES = 128
CHUNKS = 2


def dot(a, b, ca=1, cb=0, precision=None):
    return lax.dot_general(
        a, b, (((ca,), (cb,)), ((), ())), preferred_element_type=F32, precision=precision
    )


def kernel(
    n_sp,
    n_tp,
    tok_hbm,
    gain_hbm,
    w_glu_value,
    w_glu_gate,
    w_query,
    w_key,
    w_value,
    w_gate_conv,
    w_gate_attn,
    taps_hbm,
    conv_gain_hbm,
    lam_hbm,
    head_gain_hbm,
    out_conv,
    out_attn,
    out,
    w_all,
    w_out,
    tokbuf,
    acc,
    kbuf,
    vbuf,
    q4,
    m_ref,
    l_ref,
    o_ref,
    gl,
    tail_out,
    tail_in,
    sq_out,
    sq_in,
    ybuf,
    a_out,
    a_own,
    a_in,
    x_out,
    x_in,
    b_out,
    b_own,
    b_in,
    w_sem,
    tok_send,
    tok_recv,
    kv_recv,
    up_send,
    side_send,
    tail_sem,
    sq_send,
    sq_recv,
    a_sem,
    x_sem,
    b_sem,
    gain32,
    tok,
    gain,
    taps_ref,
    conv_gain,
    lam,
    head_gain,
    ga,
    small_sem,
):
    rows, depth = tok.shape
    width = depth * n_tp
    s = lax.axis_index("sp")
    t = lax.axis_index("tp")
    core = t % 2
    p1 = t + 1 - 2 * core
    p2 = (t + 2) % n_tp
    p3 = (p1 + 2) % n_tp
    y = s % 2
    z = s // 2
    mate = s + 1 - 2 * y
    has_up = s + 2 < n_sp

    smalls = [
        pltpu.make_async_copy(src, dst, small_sem.at[i])
        for i, (src, dst) in enumerate((
            (tok_hbm, tok), (gain_hbm, gain), (taps_hbm, taps_ref),
            (conv_gain_hbm, conv_gain), (lam_hbm, lam), (head_gain_hbm, head_gain),
        ))
    ]
    for copy in smalls:
        copy.start()
    weights = (w_key, w_value, w_glu_value, w_glu_gate, w_query, w_gate_conv, w_gate_attn)
    spans = []
    at = 0
    loads = []
    for i, w in enumerate(weights):
        cols = w.shape[1]
        spans.append((at, at + cols))
        loads.append(pltpu.make_async_copy(w, w_all.at[:, at : at + cols], w_sem.at[i]))
        at += cols
    total_cols = at
    at = 0
    out_loads = []
    for i, w in enumerate((out_conv, out_attn)):
        r = w.shape[0]
        out_loads.append(
            pltpu.make_async_copy(w, w_out.at[at : at + r, :], w_sem.at[len(weights) + i])
        )
        at += r
    for copy in loads + out_loads:
        copy.start()

    def tp_copy(src, dst, send, recv, to):
        return pltpu.make_async_remote_copy(
            src_ref=src, dst_ref=dst, send_sem=send, recv_sem=recv,
            device_id={"tp": to}, device_id_type=MESH,
        )

    def sp_copy(src, dst, send, recv, to):
        return pltpu.make_async_remote_copy(
            src_ref=src, dst_ref=dst, send_sem=send, recv_sem=recv,
            device_id={"sp": to}, device_id_type=MESH,
        )

    barrier = pltpu.get_barrier_semaphore()
    for peer in (p1, p2, p3):
        pl.semaphore_signal(barrier, inc=1, device_id={"tp": peer}, device_id_type=MESH)
    for by in (-2, -1, 1, 2):
        other = s + by

        @pl.when((other >= 0) & (other < n_sp))
        def _():
            pl.semaphore_signal(barrier, inc=1, device_id={"sp": other}, device_id_type=MESH)

    pl.semaphore_wait(barrier, 3 + jnp.minimum(s, 2) + jnp.minimum(n_sp - 1 - s, 2))

    for copy in smalls:
        copy.wait()

    half = rows // 2
    across = [
        tp_copy(
            tok.at[c * half : (c + 1) * half], tokbuf.at[1, c * half : (c + 1) * half],
            tok_send.at[c], tok_recv.at[c], p2,
        )
        for c in range(2)
    ]
    beside = tp_copy(tok, tokbuf.at[0], tok_send.at[2], tok_recv.at[2], p1)
    passed = [
        tp_copy(
            tokbuf.at[1, c * half : (c + 1) * half], tokbuf.at[2, c * half : (c + 1) * half],
            tok_send.at[3 + c], tok_recv.at[3 + c], p1,
        )
        for c in range(2)
    ]
    for copy in across:
        copy.start()
    beside.start()

    def prepare(x, owner):
        wide = x.astype(F32)
        first = pl.multiple_of(owner * depth, depth)
        lines = depth // LANES
        parts = [
            wide[:, b * LANES : (b + 1) * LANES] * gain32[pl.ds(owner * lines + b, 1), :]
            for b in range(lines)
        ]
        scaled = jnp.concatenate(parts, axis=1).astype(BF16)
        return scaled, jnp.sum(wide * wide, axis=1, keepdims=True), first

    gain32[...] = gain[...].astype(F32)
    scaled, squares, first = prepare(tok[...], t)
    for copy in loads:
        copy.wait()
    acc[...] = dot(scaled, w_all[pl.ds(first, depth), :])
    beside.wait_recv()
    scaled, more, first = prepare(tokbuf[0], p1)
    squares = squares + more
    acc[...] += dot(scaled, w_all[pl.ds(first, depth), :])
    for c in range(2):
        across[c].wait_recv()
        passed[c].start()
    scaled, more, first = prepare(tokbuf[1], p2)
    squares = squares + more
    acc[...] += dot(scaled, w_all[pl.ds(first, depth), :])
    for c in range(2):
        passed[c].wait_recv()
    scaled, more, first = prepare(tokbuf[2], p3)
    squares = squares + more
    inv_rms = lax.rsqrt(squares / width + EPSILON)
    early = spans[3][1]
    acc[:, :early] += dot(scaled, w_all[pl.ds(first, depth), :early])

    def projected(i, lo=0, hi=None):
        hi = rows if hi is None else hi
        a, b = spans[i]
        return (acc[lo:hi, a:b] * inv_rms[lo:hi]).astype(BF16)

    def glue(lo, hi):
        value = projected(2, lo, hi).astype(F32)
        gate = projected(3, lo, hi).astype(F32)
        return (value * jax.nn.sigmoid(gate)).astype(BF16)

    tail_out[...] = glue(rows - PAD, rows)
    tail = sp_copy(tail_out, tail_in, tail_sem.at[0], tail_sem.at[1], s + 1)

    @pl.when(s + 1 < n_sp)
    def _():
        tail.start()

    def chunk(j, c):
        buf = (kbuf, vbuf)[c * 2 // CHUNKS]
        size = buf.shape[1] * 2 // CHUNKS
        lo = (c % (CHUNKS // 2)) * size
        return buf.at[j, lo : lo + size]

    def up(j, c):
        ref = chunk(j, c)
        return sp_copy(ref, ref, up_send.at[j, c], kv_recv.at[j, c], s + 2)

    def side(j, c):
        ref = chunk(j, c)
        return sp_copy(ref, ref, side_send.at[j, c], kv_recv.at[j, c], mate)

    kbuf[s] = projected(0)
    vbuf[s] = jnp.transpose(projected(1).astype(F32)).astype(BF16)
    for c in range(CHUNKS):

        @pl.when(has_up)
        def _():
            up(s, c).start()

        @pl.when(y == 0)
        def _():
            side(s, c).start()

    acc[:, early:] += dot(scaled, w_all[pl.ds(first, depth), early:])
    query = projected(4).astype(F32) * (1.0 / math.sqrt(QK))
    heads = w_query.shape[1] // (2 * QK)
    lane = lax.broadcasted_iota(jnp.int32, (rows, 2 * QK), 1)
    for h in range(heads):
        qh = query[:, h * 2 * QK : (h + 1) * 2 * QK]
        for m in range(2):
            keep = (lane >= m * QK) & (lane < (m + 1) * QK)
            q4[2 * h + m] = jnp.where(keep, qh, 0.0).astype(BF16)
    gl[PAD:, :] = glue(0, rows).astype(F32)

    gate_attn = projected(6).astype(F32)
    ga[...] = gate_attn * jax.nn.sigmoid(gate_attn)

    key_pos = lax.broadcasted_iota(jnp.int32, (rows, rows), 0)
    query_pos = lax.broadcasted_iota(jnp.int32, (rows, rows), 1)
    allowed = key_pos <= query_pos
    k = kbuf[s]
    v = vbuf[s]
    for i in range(2 * heads):
        scores = jnp.where(allowed, dot(k, q4[i], 1, 1), NEG_BIG)
        top = jnp.max(scores, axis=0, keepdims=True)
        e = jnp.exp(scores - top)
        m_ref[i] = top
        l_ref[i] = jnp.sum(e, axis=0, keepdims=True)
        o_ref[i] = dot(v, e.astype(BF16))

    @pl.when(s == 0)
    def _():
        gl[:PAD, :] = jnp.zeros((PAD, gl.shape[1]), F32)

    @pl.when(s > 0)
    def _():
        tail.wait_recv()
        gl[:PAD, :] = tail_in[...].astype(F32)

    n_taps = taps_ref.shape[0]
    taps = taps_ref[...].astype(F32)
    conv = jnp.zeros((rows, gl.shape[1]), F32)
    for j in range(n_taps):
        lo = PAD - (n_taps - 1) + j
        conv = conv + gl[lo : lo + rows, :] * taps[j : j + 1, :]
    ones = jnp.ones((8, conv.shape[1]), F32)
    high = lax.Precision.HIGHEST
    sq_out[...] = dot(ones, conv * conv, 1, 1, high)
    sq_copies = [
        tp_copy(sq_out, sq_in.at[i], sq_send.at[i], sq_recv.at[i], p)
        for i, p in enumerate((p1, p2, p3))
    ]
    for copy in sq_copies:
        copy.start()

    def visit(j, i, at=slice(None)):
        scores = dot(kbuf[j], q4[i, at, :], 1, 1)
        old = m_ref[i, :, at]
        top = jnp.maximum(old, jnp.max(scores, axis=0, keepdims=True))
        factor = jnp.exp(old - top)
        e = jnp.exp(scores - top)
        m_ref[i, :, at] = top
        l_ref[i, :, at] = l_ref[i, :, at] * factor + jnp.sum(e, axis=0, keepdims=True)
        o_ref[i, :, at] = o_ref[i, :, at] * factor + dot(vbuf[j], e.astype(BF16))

    def mate_arrives(k):
        for c in range(CHUNKS):
            side(mate - 2 * k, c).wait_recv()

    def visit_mate(k, at=slice(None)):
        for i in range(2 * heads):
            visit(mate - 2 * k, i, at)

    maps = 2 * heads // CHUNKS

    def step(i, carry):
        k = i + 1
        j = s - 2 * k
        for c in range(CHUNKS):
            up(j, c).wait_recv()

            @pl.when(has_up)
            def _():
                up(j, c).start()

            side(j, c).start()

            @pl.when(k > 1)
            def _():
                for m in range(maps):
                    visit(j + 2, c * maps + m)

        @pl.when((k > 1) | (y == 1))
        def _():
            mate_arrives(k - 1)
            visit_mate(k - 1)

        return carry

    lax.fori_loop(0, z, step, 0)

    @pl.when(z > 0)
    def _():
        for i in range(2 * heads):
            visit(s - 2 * z, i)

    gate_conv = projected(5).astype(F32)
    for copy in sq_copies:
        copy.wait_recv()
    total_sq = sq_out[...] + sq_in[0] + sq_in[1] + sq_in[2]
    spread = jnp.full((8, conv.shape[1]), 0.125, F32)
    conv_all = conv.shape[1] * n_tp
    mean_sq = dot(total_sq, spread, 0, 0, high) / conv_all
    normed = conv * lax.rsqrt(mean_sq + EPSILON) * conv_gain[...]
    conv_local = conv.shape[1]
    ybuf[:, :conv_local] = (
        normed * jax.nn.sigmoid(normed) * (gate_conv * jax.nn.sigmoid(gate_conv))
    ).astype(BF16)

    part = rows // n_tp
    both = 2 * part
    far_rows = pl.ds(pl.multiple_of(p2 // 2 * both, both), both)
    near_rows = pl.ds(pl.multiple_of(t // 2 * both, both), both)
    more_keys = (z > 0) | (y == 1)

    def finish(at):
        for h in range(heads):
            first_map = o_ref[2 * h, :, at] / l_ref[2 * h, :, at]
            second_map = o_ref[2 * h + 1, :, at] / l_ref[2 * h + 1, :, at]
            o = first_map - lam[:, h : h + 1] * second_map
            n = o * lax.rsqrt(jnp.mean(o * o, axis=0, keepdims=True) + EPSILON)
            n = jnp.transpose(n) * head_gain[...] * HEAD_SCALE
            lo = h * VDIM
            ybuf[at, conv_local + lo : conv_local + lo + VDIM] = (
                n * ga[at, lo : lo + VDIM]
            ).astype(BF16)

    for copy in out_loads:
        copy.wait()

    @pl.when(more_keys)
    def _():
        mate_arrives(z)
        visit_mate(z, far_rows)

    finish(far_rows)


    def block(p):
        return ybuf[pl.ds(pl.multiple_of(p * part, part), part), :]

    cols = w_out.shape[1] // PIECES
    far = jnp.concatenate([block(p3), block(p2)], axis=0)
    a_copies = []
    for c in range(PIECES):
        r = dot(far, w_out[:, c * cols : (c + 1) * cols]).astype(BF16)
        a_out[c] = r[:part]
        a_own[c] = r[part:]
        copy = tp_copy(a_out.at[c], a_in.at[c], a_sem.at[0, c], a_sem.at[1, c], p1)
        copy.start()
        a_copies.append(copy)

    @pl.when(more_keys)
    def _():
        visit_mate(z, near_rows)

    x_copies = []
    for c in range(PIECES):
        a_copies[c].wait_recv()
        x_out[c] = (a_own[c].astype(F32) + a_in[c].astype(F32)).astype(BF16)
        copy = tp_copy(x_out.at[c], x_in.at[c], x_sem.at[0, c], x_sem.at[1, c], p2)
        copy.start()
        x_copies.append(copy)
    finish(near_rows)
    near = jnp.concatenate([block(p1), block(t)], axis=0)
    b_copies = []
    for c in range(PIECES):
        r = dot(near, w_out[:, c * cols : (c + 1) * cols]).astype(BF16)
        b_out[c] = r[:part]
        b_own[c] = r[part:]
        copy = tp_copy(b_out.at[c], b_in.at[c], b_sem.at[0, c], b_sem.at[1, c], p1)
        copy.start()
        b_copies.append(copy)
    for c in range(PIECES):
        b_copies[c].wait_recv()
        x_copies[c].wait_recv()
        out[:, c * cols : (c + 1) * cols] = (
            b_own[c].astype(F32) + b_in[c].astype(F32) + x_in[c].astype(F32)
        ).astype(BF16)

    for copy in across + [beside] + passed + sq_copies + a_copies + x_copies + b_copies:
        copy.wait_send()

    @pl.when(s + 1 < n_sp)
    def _():
        tail.wait_send()

    for c in range(CHUNKS):

        @pl.when(has_up)
        def _():
            up(s, c).wait_send()

        @pl.when(y == 0)
        def _():
            side(s, c).wait_send()

    def drain(i, carry):
        j = s - 2 * (i + 1)
        for c in range(CHUNKS):

            @pl.when(has_up)
            def _():
                up(j, c).wait_send()

            side(j, c).wait_send()
        return carry

    lax.fori_loop(0, z, drain, 0)


def local(n_sp, n_tp, *args):
    (tokens, in_gain, w_glu_value, w_glu_gate, w_query, w_key, w_value, w_gate_conv,
     w_gate_attn, conv_weight, conv_gain, lam, head_gain, out_conv, out_attn) = args
    rows, depth = tokens.shape
    width = depth * n_tp
    weights = (w_glu_value, w_glu_gate, w_query, w_key, w_value, w_gate_conv, w_gate_attn)
    total_cols = sum(w.shape[1] for w in weights)
    out_rows = out_conv.shape[0] + out_attn.shape[0]
    out_cols = out_conv.shape[1]
    conv_local = conv_weight.shape[1]
    heads = lam.shape[0]
    part = rows // n_tp
    cols = out_cols // PIECES
    vmem = pl.BlockSpec(memory_space=pltpu.VMEM)
    hbm = pl.BlockSpec(memory_space=pl.ANY)
    dma = pltpu.SemaphoreType.DMA
    piece = pltpu.VMEM((PIECES, part, cols), BF16)
    return pl.pallas_call(
        functools.partial(kernel, n_sp, n_tp),
        out_shape=jax.ShapeDtypeStruct((part, out_cols), BF16),
        in_specs=[hbm] * len(args),
        out_specs=vmem,
        scratch_shapes=[
            pltpu.VMEM((width, total_cols), BF16),
            pltpu.VMEM((out_rows, out_cols), BF16),
            pltpu.VMEM((3, rows, depth), BF16),
            pltpu.VMEM((rows, total_cols), F32),
            pltpu.VMEM((n_sp, rows, 2 * QK), BF16),
            pltpu.VMEM((n_sp, VDIM, rows), BF16),
            pltpu.VMEM((2 * heads, rows, 2 * QK), BF16),
            pltpu.VMEM((2 * heads, 1, rows), F32),
            pltpu.VMEM((2 * heads, 1, rows), F32),
            pltpu.VMEM((2 * heads, VDIM, rows), F32),
            pltpu.VMEM((PAD + rows, conv_local), F32),
            pltpu.VMEM((PAD, conv_local), BF16),
            pltpu.VMEM((PAD, conv_local), BF16),
            pltpu.VMEM((8, rows), F32),
            pltpu.VMEM((3, 8, rows), F32),
            pltpu.VMEM((rows, out_rows), BF16),
            piece, piece, piece, piece, piece, piece, piece, piece,
            dma((9,)),
            dma((5,)),
            dma((5,)),
            dma((n_sp, CHUNKS)),
            dma((n_sp, CHUNKS)),
            dma((n_sp, CHUNKS)),
            dma((2,)),
            dma((3,)),
            dma((3,)),
            dma((2, PIECES)),
            dma((2, PIECES)),
            dma((2, PIECES)),
            pltpu.VMEM((width // LANES, LANES), F32),
            pltpu.VMEM(tokens.shape, BF16),
            pltpu.VMEM((width // LANES, LANES), BF16),
            pltpu.VMEM(conv_weight.shape, BF16),
            pltpu.VMEM((1, conv_local), F32),
            pltpu.VMEM((1, heads), F32),
            pltpu.VMEM((1, VDIM), F32),
            pltpu.VMEM((rows, heads * VDIM), F32),
            dma((6,)),
        ],
        compiler_params=pltpu.CompilerParams(
            collective_id=0, has_side_effects=True, vmem_limit_bytes=60 * 1024 * 1024
        ),
    )(
        tokens, in_gain.reshape(width // LANES, LANES), w_glu_value, w_glu_gate, w_query, w_key, w_value,
        w_gate_conv, w_gate_attn, conv_weight, conv_gain.reshape(1, conv_local),
        lam.reshape(1, heads),
        head_gain.reshape(1, VDIM), out_conv, out_attn,
    )


def solution(mesh):
    n_sp, n_tp = mesh.shape["sp"], mesh.shape["tp"]
    assert n_tp == 4 and n_sp % 2 == 0
    col = P(None, "tp")
    in_specs = (
        P("sp", "tp"), P(), col, col, col, col, col, col, col, col,
        P("tp"), P("tp"), P(), P("tp", None), P("tp", None),
    )
    return jax.shard_map(
        functools.partial(local, n_sp, n_tp), mesh=mesh, in_specs=in_specs,
        out_specs=P(("sp", "tp"), None), check_vma=False,
    )
```

```python
import functools
import math

import jax
import jax.numpy as jnp
from jax import lax
from jax.experimental import pallas as pl
from jax.experimental.pallas import tpu as pltpu
from jax.sharding import PartitionSpec as P

EPSILON = 1e-06
NEG_BIG = -1e30
HEAD_SCALE = 0.8
QK = 64
VDIM = 128
MESH = pl.DeviceIdType.MESH
F32 = jnp.float32
BF16 = jnp.bfloat16
PIECES = 4
PAD = 32
LANES = 128
CHUNKS = 2


def dot(a, b, ca=1, cb=0, precision=None):
    return lax.dot_general(
        a, b, (((ca,), (cb,)), ((), ())), preferred_element_type=F32, precision=precision
    )


def kernel(
    n_sp,
    n_tp,
    tok_hbm,
    gain_hbm,
    w_glu_value,
    w_glu_gate,
    w_query,
    w_key,
    w_value,
    w_gate_conv,
    w_gate_attn,
    taps_hbm,
    conv_gain_hbm,
    lam_hbm,
    head_gain_hbm,
    out_conv,
    out_attn,
    out,
    w_all,
    w_out,
    tokbuf,
    acc,
    kv,
    q4,
    m_ref,
    l_ref,
    o_ref,
    gl,
    tail_out,
    tail_in,
    sq_out,
    sq_in,
    ybuf,
    a_out,
    a_own,
    a_in,
    x_out,
    x_in,
    b_out,
    b_own,
    b_in,
    w_sem,
    tok_send,
    tok_recv,
    kv_recv,
    up_send,
    side_send,
    tail_sem,
    sq_send,
    sq_recv,
    a_sem,
    x_sem,
    b_sem,
    gain32,
    tok,
    gain,
    taps_ref,
    conv_gain,
    lam,
    head_gain,
    ga,
    small_sem,
):
    rows, depth = tok.shape
    assert rows == 2 * CHUNKS * QK
    width = depth * n_tp
    s = lax.axis_index("sp")
    t = lax.axis_index("tp")
    core = t % 2
    p1 = t + 1 - 2 * core
    p2 = (t + 2) % n_tp
    p3 = (p1 + 2) % n_tp
    y = s % 2
    z = s // 2
    mate = s + 1 - 2 * y
    has_up = s + 2 < n_sp

    smalls = [
        pltpu.make_async_copy(src, dst, small_sem.at[i])
        for i, (src, dst) in enumerate((
            (tok_hbm, tok), (gain_hbm, gain), (taps_hbm, taps_ref),
            (conv_gain_hbm, conv_gain), (lam_hbm, lam), (head_gain_hbm, head_gain),
        ))
    ]
    for copy in smalls:
        copy.start()
    weights = (w_key, w_value, w_glu_value, w_glu_gate, w_query, w_gate_conv, w_gate_attn)
    spans = []
    at = 0
    loads = []
    for i, w in enumerate(weights):
        cols = w.shape[1]
        spans.append((at, at + cols))
        loads.append(pltpu.make_async_copy(w, w_all.at[:, at : at + cols], w_sem.at[i]))
        at += cols
    total_cols = at
    at = 0
    out_loads = []
    for i, w in enumerate((out_conv, out_attn)):
        r = w.shape[0]
        out_loads.append(
            pltpu.make_async_copy(w, w_out.at[at : at + r, :], w_sem.at[len(weights) + i])
        )
        at += r
    for copy in loads + out_loads:
        copy.start()

    def tp_copy(src, dst, send, recv, to):
        return pltpu.make_async_remote_copy(
            src_ref=src, dst_ref=dst, send_sem=send, recv_sem=recv,
            device_id={"tp": to}, device_id_type=MESH,
        )

    def sp_copy(src, dst, send, recv, to):
        return pltpu.make_async_remote_copy(
            src_ref=src, dst_ref=dst, send_sem=send, recv_sem=recv,
            device_id={"sp": to}, device_id_type=MESH,
        )

    barrier = pltpu.get_barrier_semaphore()
    for peer in (p1, p2, p3):
        pl.semaphore_signal(barrier, inc=1, device_id={"tp": peer}, device_id_type=MESH)
    n_z = n_sp // 2
    reach = range(2, n_sp, 4)
    for by in [-1, 1] + [-d for d in reach] + list(reach):
        other = s + by

        @pl.when((other >= 0) & (other < n_sp))
        def _():
            pl.semaphore_signal(barrier, inc=1, device_id={"sp": other}, device_id_type=MESH)

    above = (n_z - z) // 2
    pl.semaphore_wait(
        barrier,
        3 + jnp.minimum(s, 1) + jnp.minimum(n_sp - 1 - s, 1) + (z + 1) // 2 + above,
    )

    for copy in smalls:
        copy.wait()

    half = rows // 2
    across = [
        tp_copy(
            tok.at[c * half : (c + 1) * half], tokbuf.at[1, c * half : (c + 1) * half],
            tok_send.at[c], tok_recv.at[c], p2,
        )
        for c in range(2)
    ]
    beside = tp_copy(tok, tokbuf.at[0], tok_send.at[2], tok_recv.at[2], p1)
    passed = [
        tp_copy(
            tokbuf.at[1, c * half : (c + 1) * half], tokbuf.at[2, c * half : (c + 1) * half],
            tok_send.at[3 + c], tok_recv.at[3 + c], p1,
        )
        for c in range(2)
    ]
    for copy in across:
        copy.start()
    beside.start()

    def prepare(x, owner):
        wide = x.astype(F32)
        first = pl.multiple_of(owner * depth, depth)
        lines = depth // LANES
        parts = [
            wide[:, b * LANES : (b + 1) * LANES] * gain32[pl.ds(owner * lines + b, 1), :]
            for b in range(lines)
        ]
        scaled = jnp.concatenate(parts, axis=1).astype(BF16)
        return scaled, jnp.sum(wide * wide, axis=1, keepdims=True), first

    gain32[...] = gain[...].astype(F32)
    scaled, squares, first = prepare(tok[...], t)
    for copy in loads:
        copy.wait()
    acc[...] = dot(scaled, w_all[pl.ds(first, depth), :])
    beside.wait_recv()
    scaled, more, first = prepare(tokbuf[0], p1)
    squares = squares + more
    acc[...] += dot(scaled, w_all[pl.ds(first, depth), :])
    early = spans[3][1]
    invs, scaled2, scaled3 = [], [], []

    def projected(i, lo=0, hi=None):
        hi = rows if hi is None else hi
        a, b = spans[i]
        inv = jnp.concatenate(invs, axis=0)[lo:hi]
        return (acc[lo:hi, a:b] * inv).astype(BF16)

    def glue(lo, hi):
        value = projected(2, lo, hi).astype(F32)
        gate = projected(3, lo, hi).astype(F32)
        return (value * jax.nn.sigmoid(gate)).astype(BF16)

    tail = sp_copy(tail_out, tail_in, tail_sem.at[0], tail_sem.at[1], s + 1)

    def up(j, c):
        ref = kv.at[j, c]
        return sp_copy(ref, ref, up_send.at[j, c], kv_recv.at[j, c], s + 2)

    def ahead(i, c):
        ref = kv.at[s, c]
        to = s + 2 + 4 * i
        return sp_copy(ref, ref, up_send.at[to, c], kv_recv.at[s, c], to)

    def side(j, c):
        ref = kv.at[j, c]
        return sp_copy(ref, ref, side_send.at[j, c], kv_recv.at[j, c], mate)

    for c in range(CHUNKS):
        at = slice(c * half, (c + 1) * half)
        across[c].wait_recv()
        passed[c].start()
        x2, more2, first2 = prepare(tokbuf[1, at], p2)
        acc[at, :early] += dot(x2, w_all[pl.ds(first2, depth), :early])
        passed[c].wait_recv()
        x3, more3, first3 = prepare(tokbuf[2, at], p3)
        acc[at, :early] += dot(x3, w_all[pl.ds(first3, depth), :early])
        scaled2.append(x2)
        scaled3.append(x3)
        invs.append(lax.rsqrt((squares[at] + more2 + more3) / width + EPSILON))
        if c == CHUNKS - 1:
            tail_out[...] = glue(rows - PAD, rows)

            @pl.when(s + 1 < n_sp)
            def _():
                tail.start()

        kv[s, c, :half] = projected(0, c * half, (c + 1) * half)
        kv[s, c, half:] = jnp.transpose(
            projected(1, c * half, (c + 1) * half).astype(F32)
        ).astype(BF16)

        def send_ahead(i, carry):
            ahead(i, c).start()
            return carry

        lax.fori_loop(0, above, send_ahead, 0)

        @pl.when(y == 0)
        def _():
            side(s, c).start()

    def keys(j):
        return jnp.concatenate([kv[j, c, :half] for c in range(CHUNKS)], axis=0)

    def values(j):
        return jnp.concatenate([kv[j, c, half:] for c in range(CHUNKS)], axis=1)

    for parts, first in ((scaled2, first2), (scaled3, first3)):
        acc[:, early:] += dot(
            jnp.concatenate(parts, axis=0), w_all[pl.ds(first, depth), early:]
        )
    query = projected(4).astype(F32) * (1.0 / math.sqrt(QK))
    heads = w_query.shape[1] // (2 * QK)
    lane = lax.broadcasted_iota(jnp.int32, (rows, 2 * QK), 1)
    for h in range(heads):
        qh = query[:, h * 2 * QK : (h + 1) * 2 * QK]
        for m in range(2):
            keep = (lane >= m * QK) & (lane < (m + 1) * QK)
            q4[2 * h + m] = jnp.where(keep, qh, 0.0).astype(BF16)
    gl[PAD:, :] = glue(0, rows).astype(F32)

    gate_attn = projected(6).astype(F32)
    ga[...] = gate_attn * jax.nn.sigmoid(gate_attn)

    key_pos = lax.broadcasted_iota(jnp.int32, (rows, rows), 0)
    query_pos = lax.broadcasted_iota(jnp.int32, (rows, rows), 1)
    allowed = key_pos <= query_pos
    k = keys(s)
    v = values(s)
    for i in range(2 * heads):
        scores = jnp.where(allowed, dot(k, q4[i], 1, 1), NEG_BIG)
        top = jnp.max(scores, axis=0, keepdims=True)
        e = jnp.exp(scores - top)
        m_ref[i] = top
        l_ref[i] = jnp.sum(e, axis=0, keepdims=True)
        o_ref[i] = dot(v, e.astype(BF16))

    @pl.when(s == 0)
    def _():
        gl[:PAD, :] = jnp.zeros((PAD, gl.shape[1]), F32)

    @pl.when(s > 0)
    def _():
        tail.wait_recv()
        gl[:PAD, :] = tail_in[...].astype(F32)

    n_taps = taps_ref.shape[0]
    taps = taps_ref[...].astype(F32)
    conv = jnp.zeros((rows, gl.shape[1]), F32)
    for j in range(n_taps):
        lo = PAD - (n_taps - 1) + j
        conv = conv + gl[lo : lo + rows, :] * taps[j : j + 1, :]
    ones = jnp.ones((8, conv.shape[1]), F32)
    high = lax.Precision.HIGHEST
    sq_out[...] = dot(ones, conv * conv, 1, 1, high)
    sq_copies = [
        tp_copy(sq_out, sq_in.at[i], sq_send.at[i], sq_recv.at[i], p)
        for i, p in enumerate((p1, p2, p3))
    ]
    for copy in sq_copies:
        copy.start()

    def visit(j, i, at=slice(None)):
        scores = dot(keys(j), q4[i, at, :], 1, 1)
        old = m_ref[i, :, at]
        top = jnp.maximum(old, jnp.max(scores, axis=0, keepdims=True))
        factor = jnp.exp(old - top)
        e = jnp.exp(scores - top)
        m_ref[i, :, at] = top
        l_ref[i, :, at] = l_ref[i, :, at] * factor + jnp.sum(e, axis=0, keepdims=True)
        o_ref[i, :, at] = o_ref[i, :, at] * factor + dot(values(j), e.astype(BF16))

    def mate_arrives(k):
        for c in range(CHUNKS):
            side(mate - 2 * k, c).wait_recv()

    def visit_mate(k, at=slice(None)):
        for i in range(2 * heads):
            visit(mate - 2 * k, i, at)

    maps = 2 * heads // CHUNKS

    def step(i, carry):
        k = i + 1
        j = s - 2 * k
        for c in range(CHUNKS):
            up(j, c).wait_recv()

            @pl.when(has_up & (k % 2 == 1))
            def _():
                up(j, c).start()

            side(j, c).start()

            @pl.when(k > 1)
            def _():
                for m in range(maps):
                    visit(j + 2, c * maps + m)

        @pl.when((k > 1) | (y == 1))
        def _():
            mate_arrives(k - 1)
            visit_mate(k - 1)

        return carry

    lax.fori_loop(0, z, step, 0)

    @pl.when(z > 0)
    def _():
        for i in range(2 * heads):
            visit(s - 2 * z, i)

    gate_conv = projected(5).astype(F32)
    for copy in sq_copies:
        copy.wait_recv()
    total_sq = sq_out[...] + sq_in[0] + sq_in[1] + sq_in[2]
    spread = jnp.full((8, conv.shape[1]), 0.125, F32)
    conv_all = conv.shape[1] * n_tp
    mean_sq = dot(total_sq, spread, 0, 0, high) / conv_all
    normed = conv * lax.rsqrt(mean_sq + EPSILON) * conv_gain[...]
    conv_local = conv.shape[1]
    ybuf[:, :conv_local] = (
        normed * jax.nn.sigmoid(normed) * (gate_conv * jax.nn.sigmoid(gate_conv))
    ).astype(BF16)

    part = rows // n_tp
    both = 2 * part
    far_rows = pl.ds(pl.multiple_of(p2 // 2 * both, both), both)
    near_rows = pl.ds(pl.multiple_of(t // 2 * both, both), both)
    more_keys = (z > 0) | (y == 1)

    def finish(at):
        for h in range(heads):
            first_map = o_ref[2 * h, :, at] / l_ref[2 * h, :, at]
            second_map = o_ref[2 * h + 1, :, at] / l_ref[2 * h + 1, :, at]
            o = first_map - lam[:, h : h + 1] * second_map
            n = o * lax.rsqrt(jnp.mean(o * o, axis=0, keepdims=True) + EPSILON)
            n = jnp.transpose(n) * head_gain[...] * HEAD_SCALE
            lo = h * VDIM
            ybuf[at, conv_local + lo : conv_local + lo + VDIM] = (
                n * ga[at, lo : lo + VDIM]
            ).astype(BF16)

    for copy in out_loads:
        copy.wait()

    @pl.when(more_keys)
    def _():
        mate_arrives(z)
        visit_mate(z, far_rows)

    finish(far_rows)


    def block(p):
        return ybuf[pl.ds(pl.multiple_of(p * part, part), part), :]

    cols = w_out.shape[1] // PIECES
    far = jnp.concatenate([block(p3), block(p2)], axis=0)
    a_copies = []
    for c in range(PIECES):
        r = dot(far, w_out[:, c * cols : (c + 1) * cols]).astype(BF16)
        a_out[c] = r[:part]
        a_own[c] = r[part:]
        copy = tp_copy(a_out.at[c], a_in.at[c], a_sem.at[0, c], a_sem.at[1, c], p1)
        copy.start()
        a_copies.append(copy)

    @pl.when(more_keys)
    def _():
        visit_mate(z, near_rows)

    x_copies = []
    for c in range(PIECES):
        a_copies[c].wait_recv()
        x_out[c] = (a_own[c].astype(F32) + a_in[c].astype(F32)).astype(BF16)
        copy = tp_copy(x_out.at[c], x_in.at[c], x_sem.at[0, c], x_sem.at[1, c], p2)
        copy.start()
        x_copies.append(copy)
    finish(near_rows)
    near = jnp.concatenate([block(p1), block(t)], axis=0)
    b_copies = []
    for c in range(PIECES):
        r = dot(near, w_out[:, c * cols : (c + 1) * cols]).astype(BF16)
        b_out[c] = r[:part]
        b_own[c] = r[part:]
        copy = tp_copy(b_out.at[c], b_in.at[c], b_sem.at[0, c], b_sem.at[1, c], p1)
        copy.start()
        b_copies.append(copy)
    for c in range(PIECES):
        b_copies[c].wait_recv()
        x_copies[c].wait_recv()
        out[:, c * cols : (c + 1) * cols] = (
            b_own[c].astype(F32) + b_in[c].astype(F32) + x_in[c].astype(F32)
        ).astype(BF16)

    for copy in across + [beside] + passed + sq_copies + a_copies + x_copies + b_copies:
        copy.wait_send()

    @pl.when(s + 1 < n_sp)
    def _():
        tail.wait_send()

    for c in range(CHUNKS):

        def sent_ahead(i, carry):
            ahead(i, c).wait_send()
            return carry

        lax.fori_loop(0, above, sent_ahead, 0)

        @pl.when(y == 0)
        def _():
            side(s, c).wait_send()

    def drain(i, carry):
        j = s - 2 * (i + 1)
        for c in range(CHUNKS):

            @pl.when(has_up & (i % 2 == 0))
            def _():
                up(j, c).wait_send()

            side(j, c).wait_send()
        return carry

    lax.fori_loop(0, z, drain, 0)


def local(n_sp, n_tp, *args):
    (tokens, in_gain, w_glu_value, w_glu_gate, w_query, w_key, w_value, w_gate_conv,
     w_gate_attn, conv_weight, conv_gain, lam, head_gain, out_conv, out_attn) = args
    rows, depth = tokens.shape
    width = depth * n_tp
    weights = (w_glu_value, w_glu_gate, w_query, w_key, w_value, w_gate_conv, w_gate_attn)
    total_cols = sum(w.shape[1] for w in weights)
    out_rows = out_conv.shape[0] + out_attn.shape[0]
    out_cols = out_conv.shape[1]
    conv_local = conv_weight.shape[1]
    heads = lam.shape[0]
    part = rows // n_tp
    cols = out_cols // PIECES
    vmem = pl.BlockSpec(memory_space=pltpu.VMEM)
    hbm = pl.BlockSpec(memory_space=pl.ANY)
    dma = pltpu.SemaphoreType.DMA
    piece = pltpu.VMEM((PIECES, part, cols), BF16)
    return pl.pallas_call(
        functools.partial(kernel, n_sp, n_tp),
        out_shape=jax.ShapeDtypeStruct((part, out_cols), BF16),
        in_specs=[hbm] * len(args),
        out_specs=vmem,
        scratch_shapes=[
            pltpu.VMEM((width, total_cols), BF16),
            pltpu.VMEM((out_rows, out_cols), BF16),
            pltpu.VMEM((3, rows, depth), BF16),
            pltpu.VMEM((rows, total_cols), F32),
            pltpu.VMEM((n_sp, CHUNKS, rows // CHUNKS + VDIM, 2 * QK), BF16),
            pltpu.VMEM((2 * heads, rows, 2 * QK), BF16),
            pltpu.VMEM((2 * heads, 1, rows), F32),
            pltpu.VMEM((2 * heads, 1, rows), F32),
            pltpu.VMEM((2 * heads, VDIM, rows), F32),
            pltpu.VMEM((PAD + rows, conv_local), F32),
            pltpu.VMEM((PAD, conv_local), BF16),
            pltpu.VMEM((PAD, conv_local), BF16),
            pltpu.VMEM((8, rows), F32),
            pltpu.VMEM((3, 8, rows), F32),
            pltpu.VMEM((rows, out_rows), BF16),
            piece, piece, piece, piece, piece, piece, piece, piece,
            dma((9,)),
            dma((5,)),
            dma((5,)),
            dma((n_sp, CHUNKS)),
            dma((n_sp, CHUNKS)),
            dma((n_sp, CHUNKS)),
            dma((2,)),
            dma((3,)),
            dma((3,)),
            dma((2, PIECES)),
            dma((2, PIECES)),
            dma((2, PIECES)),
            pltpu.VMEM((width // LANES, LANES), F32),
            pltpu.VMEM(tokens.shape, BF16),
            pltpu.VMEM((width // LANES, LANES), BF16),
            pltpu.VMEM(conv_weight.shape, BF16),
            pltpu.VMEM((1, conv_local), F32),
            pltpu.VMEM((1, heads), F32),
            pltpu.VMEM((1, VDIM), F32),
            pltpu.VMEM((rows, heads * VDIM), F32),
            dma((6,)),
        ],
        compiler_params=pltpu.CompilerParams(
            collective_id=0, has_side_effects=True, vmem_limit_bytes=60 * 1024 * 1024
        ),
    )(
        tokens, in_gain.reshape(width // LANES, LANES), w_glu_value, w_glu_gate, w_query, w_key, w_value,
        w_gate_conv, w_gate_attn, conv_weight, conv_gain.reshape(1, conv_local),
        lam.reshape(1, heads),
        head_gain.reshape(1, VDIM), out_conv, out_attn,
    )


def solution(mesh):
    n_sp, n_tp = mesh.shape["sp"], mesh.shape["tp"]
    assert n_tp == 4 and n_sp % 2 == 0
    col = P(None, "tp")
    in_specs = (
        P("sp", "tp"), P(), col, col, col, col, col, col, col, col,
        P("tp"), P("tp"), P(), P("tp", None), P("tp", None),
    )
    return jax.shard_map(
        functools.partial(local, n_sp, n_tp), mesh=mesh, in_specs=in_specs,
        out_specs=P(("sp", "tp"), None), check_vma=False,
    )
```
